32 devices in a mesh: ep: 4 (over y, x), tp: 8 (over z, core).
Axes of the slice: x: 2, y: 2, z: 4, core: 2. Of those that a mesh axis runs over, the one named last changes fastest.
Arguments:
- queries: bfloat16 [3072, 2048], P('ep', 'tp'), may hold values from -6 to 6
- keys: bfloat16 [3072, 512], P('ep'), may hold values from -6 to 6
- values: bfloat16 [3072, 512], P('ep'), may hold values from -6 to 6
- query_gain: float32 [128], replicated, may hold values from 1 to 4.5
- key_gain: float32 [128], replicated, may hold values from 1 to 4.5
- out_weight: bfloat16 [2048, 2048], P('tp'), may hold values from -0.75 to 0.75
- tokens_b: bfloat16 [1536, 2048], P('ep'), may hold values from -6 to 6
- norm_gain: float32 [2048], replicated, may hold values from 0.1 to 1.9
- routes: int32 [1536, 2], P('ep'), may hold values from 0 to 15, all different within a row; in each aligned block of 48 rows (0 to 47, 48 to 95, ...) at most 8 rows name the same one
- route_weight: float32 [1536, 2], P('ep'), may hold values from 0.2 to 1
- gate_weight: bfloat16 [16, 2048, 4096], P('ep', None, 'tp'), may hold values from -0.125 to 0.125
- up_weight: bfloat16 [16, 2048, 4096], P('ep', None, 'tp'), may hold values from -0.125 to 0.125
- down_weight: bfloat16 [16, 4096, 2048], P('ep', 'tp'), may hold values from -0.09375 to 0.09375
Outputs:
- mixed_out: bfloat16 [3072, 2048], P(('ep', 'tp'))
- expert_out: bfloat16 [1536, 2048], P(('ep', 'tp'))
The draws below stay inside these ranges and needn't reach their ends.
Inputs may be any that keep to these rules, and one draw needn't show every extreme that they name: `routes`: A row names 2 different experts. In each aligned block of 48 rows no expert is named more than 8 times, a bound that some block reaches.
All inputs are finite; a program needn't handle non-finite values.
Results may differ from the reference program's by a relative error of at most 0.019.
Values may be sent and summed in bfloat16 or wider, within the bound.
A program may use at most 128 MiB of HBM per device.

```python
import math
import jax
import jax.numpy as jnp
import numpy as np
from jax import lax

D = 2048
HD = 128
HQ = 16
KVH = 4
GROUP = 4
FF = 4096
EXPERTS = 16
TOPK = 2
GRID_W = 64
TOK_DEV = 48
CAP = 8
LEN = 3072
TOKB = 1536
N_TP = 8


def draw_queries(key, part):
    drawn = jax.random.normal(jax.random.fold_in(key, 11), (LEN, HQ, HD), jnp.float32)
    return jnp.clip(drawn, -6.0, 6.0).reshape(LEN, HQ * HD).astype(jnp.bfloat16)


def draw_keys(key, part):
    drawn = jax.random.normal(jax.random.fold_in(key, 12), (LEN, KVH, HD), jnp.float32)
    return jnp.clip(drawn, -6.0, 6.0).reshape(LEN, KVH * HD).astype(jnp.bfloat16)


def draw_query_gain(key, part):
    uniform_g = jax.random.uniform(jax.random.fold_in(key, 13), (HD,), jnp.float32, 1.0, 2.0)
    return uniform_g


def draw_key_gain(key, part):
    uniform_g = jax.random.uniform(jax.random.fold_in(key, 14), (HD,), jnp.float32, 1.0, 2.0)
    return uniform_g


def block_scale(key, dims, pieces, smallest, top_value):
    level, own = 1.0, jax.random.fold_in(key, 6)
    for position, shards_of in pieces:
        steps = jnp.exp(jax.random.uniform(jax.random.fold_in(own, position), (shards_of,), jnp.float32, smallest / len(pieces), top_value / len(pieces)))
        level = level * jnp.repeat(steps, dims[position] // shards_of).reshape([-1 if axis == position else 1 for axis in range(len(dims))])
    return level


def deal_out(rng, own, number, rows, count, top, most, lean):
    sequence = jax.random.permutation(rng, count)
    heavy_load, common = load_shares(count, rows * top, most, lean, True), load_shares(count, rows * top, most, lean, False)
    places = jnp.arange(count)

    def named(sizes, rotation):
        used = int((sizes > 0).sum())
        fixed = max(1, used // 4)
        moved = fixed + (places - fixed + rotation * (used - fixed)) % max(1, count - fixed)
        return jnp.zeros((count,), jnp.int32).at[sequence[jnp.where(places < fixed, places, moved)]].set(jnp.asarray(sizes, jnp.int32))

    sizes = jnp.where(number % 4 == 0, named(heavy_load, number // 4), named(common, number - number // 4 - 1))
    mixed = jax.random.permutation(jax.random.fold_in(own, 3), count)
    donor, sink = mixed[0:count // 2 * 2:2], mixed[1:count // 2 * 2:2]
    room = jnp.minimum(sizes[donor] - 1, most - sizes[sink]) // 2
    room = jnp.where((donor == sequence[0]) | (sink == sequence[0]) | (sizes[sink] == 0), 0, jnp.maximum(room, 0))
    moved = jax.random.randint(jax.random.fold_in(own, 4), (count // 2,), 0, 1 << 20) % (room + 1)
    sizes = sizes.at[donor].add(-moved).at[sink].add(moved)
    labels = jnp.searchsorted(jnp.cumsum(sizes), jnp.arange(rows * top), side="right").astype(jnp.int32)
    table = labels.reshape(top, rows).T
    table = table[jax.random.permutation(jax.random.fold_in(own, 1), rows)]
    rotation = jax.random.randint(jax.random.fold_in(own, 2), (rows, 1), 0, top)
    return jnp.take_along_axis(table, (jnp.arange(top)[None, :] + rotation) % top, axis=1)


def load_shares(amount, total, most, slope, full):
    weights = [(1 << 20) // math.isqrt(grade ** slope) + 1 for grade in range(1, amount + 1)]
    largest = most if full else min(most, max(-(-total // amount), total * weights[0] // sum(weights)))
    least = 1 if total - largest >= amount - 1 else 0
    counts, rest = [largest] + [least] * (amount - 1), total - largest - least * (amount - 1)
    while rest > 0:
        movable = [i for i in range(1, amount) if counts[i] < largest] or [i for i in range(1, amount) if counts[i] < most]
        pool, budget = sum([weights[i] for i in movable]), rest
        for i in movable:
            extra = min(most - counts[i], max(1, budget * weights[i] // pool), rest)
            counts[i] = counts[i] + extra
            rest = rest - extra
    return np.array(counts)


def noise(own_key, shape, deviation, limit, pieces=(), kind=jnp.bfloat16):
    entries = jax.random.normal(own_key, shape, jnp.float32) * deviation
    if len(pieces) > 0:
        entries = block_scale(own_key, shape, pieces, -0.22, 0.18) * entries
    return jnp.clip(entries, min=-limit, max=limit).astype(kind)


def setup_inputs(seed: int = 0) -> dict:
    arg_keys = jax.random.split(jax.random.key(seed), 14)
    queries = draw_queries(jax.random.fold_in(arg_keys[13], 71), 0)
    keys = draw_keys(jax.random.fold_in(arg_keys[13], 71), 0)
    values = noise(arg_keys[2], (LEN, KVH * HD), 1.0, 6.0, ((0, 4),))
    query_gain = draw_query_gain(jax.random.fold_in(arg_keys[13], 71), 0)
    key_gain = draw_key_gain(jax.random.fold_in(arg_keys[13], 71), 0)
    out_weight = noise(arg_keys[5], (HQ * HD, D), (HD // 2) ** -0.5, 0.75, ((0, 8),))
    tokens_b = noise(arg_keys[6], (TOKB, D), 1.0, 6.0, ((0, 4),))
    norm_gain = jnp.clip(1.0 + 0.18 * jax.random.normal(arg_keys[7], (D,), jnp.float32), 0.1, 1.9)
    routes_keys = jax.random.split(jax.random.fold_in(arg_keys[8], 1), TOKB // TOK_DEV)
    routes_turns = jax.random.permutation(jax.random.fold_in(arg_keys[8], 3), TOKB // TOK_DEV)
    routes = jax.vmap(lambda own, number: deal_out(jax.random.fold_in(arg_keys[8], 2), own, number, TOK_DEV, EXPERTS, TOPK, CAP, 1))(routes_keys, routes_turns).reshape((TOKB, TOPK))
    route_weight = jnp.clip(jnp.exp(math.log(1.0) - 1.609438 * jax.random.uniform(arg_keys[9], (TOKB, TOPK), jnp.float32) ** block_scale(arg_keys[9], (TOKB, TOPK), ((0, 4),), -0.2, 0.2)), 0.2, 1.0)
    gate_weight = noise(arg_keys[10], (EXPERTS, D, FF), D ** -0.5, 0.125, ((0, 4), (2, 8)))
    up_weight = noise(arg_keys[11], (EXPERTS, D, FF), D ** -0.5, 0.125, ((0, 4), (2, 8)))
    down_weight = noise(arg_keys[12], (EXPERTS, FF, D), FF ** -0.5, 0.09375, ((0, 4), (1, 8)))
    return dict(queries=queries, keys=keys, values=values, query_gain=query_gain, key_gain=key_gain, out_weight=out_weight, tokens_b=tokens_b, norm_gain=norm_gain, routes=routes, route_weight=route_weight, gate_weight=gate_weight, up_weight=up_weight, down_weight=down_weight)


EPS = 1e-06
THETA = 10000.0
q_block = 64

def rotate(field, positions):
    n_freq = HD // 4
    row_pos = (positions // GRID_W).astype(jnp.float32)
    col_pos = (positions % GRID_W).astype(jnp.float32)
    inverse = THETA ** (-jnp.arange(n_freq, dtype=jnp.float32) / n_freq)
    angles = jnp.stack([row_pos[:, None] * inverse, col_pos[:, None] * inverse], axis=1)
    cosine = jnp.cos(angles)[:, None]
    sine = jnp.sin(angles)[:, None]
    length, n_heads = (field.shape[0], field.shape[1])
    halves = field.reshape(length, n_heads, 2, 2, n_freq)
    leading = halves[..., 0, :]
    second = halves[..., 1, :]
    turned = jnp.stack([leading * cosine - second * sine, second * cosine + leading * sine], axis=-2)
    return turned.reshape(length, n_heads, HD)

def prepare(source, gain_vec, positions, n_heads):
    length = source.shape[0]
    field = source.astype(jnp.float32).reshape(length, n_heads, HD)
    field = field * lax.rsqrt(lax.optimization_barrier(jnp.mean(field * field, axis=-1, keepdims=True)) + EPS) * gain_vec.astype(jnp.float32)
    return rotate(field, positions).astype(jnp.bfloat16)

def attend_block(query_blk, key_t, value_h):
    scores = jnp.einsum('qkgd,skd->kgqs', query_blk.astype(jnp.float32), key_t.astype(jnp.float32)) * HD ** (-0.5)
    row_max = lax.optimization_barrier(jnp.max(scores, axis=-1, keepdims=True))
    weights = jnp.exp(scores - row_max)
    totals = lax.optimization_barrier(jnp.sum(weights, axis=-1, keepdims=True))
    rounded = lax.optimization_barrier(weights.astype(jnp.bfloat16))
    merged = jnp.einsum('kgqs,skd->kgqd', rounded.astype(jnp.float32), value_h.astype(jnp.float32)) / totals
    return jnp.transpose(merged, (2, 0, 1, 3)).reshape(query_blk.shape[0], HQ * HD).astype(jnp.bfloat16)

def reference(queries, keys, values, query_gain, key_gain, out_weight, tokens_b, norm_gain, routes, route_weight, gate_weight, up_weight, down_weight):
    positions = jnp.arange(LEN, dtype=jnp.int32)
    query_t = prepare(queries, query_gain, positions, HQ).reshape(LEN // q_block, q_block, KVH, GROUP, HD)
    key_t = prepare(keys, key_gain, positions, KVH)
    value_h = values.reshape(LEN, KVH, HD)
    attended = lax.map(lambda query_blk: attend_block(query_blk, key_t, value_h), query_t).reshape(LEN, HQ * HD)
    mixed_out = jnp.dot(attended, out_weight, preferred_element_type=jnp.float32).astype(jnp.bfloat16)
    n_tokens = tokens_b.shape[0]
    n_blocks = n_tokens // TOK_DEV
    field = tokens_b.astype(jnp.float32)
    normed = (field * lax.rsqrt(lax.optimization_barrier(jnp.mean(field * field, axis=-1, keepdims=True)) + EPS) * norm_gain.astype(jnp.float32)).astype(jnp.bfloat16)
    assigned = routes.reshape(n_blocks, TOK_DEV * TOPK)
    onehot = (assigned[:, :, None] == jnp.arange(EXPERTS, dtype=jnp.int32)[None, None, :]).astype(jnp.int32)
    slot_rank = lax.optimization_barrier(jnp.sum((jnp.cumsum(onehot, axis=1) - onehot) * onehot, axis=-1))
    block_ids = jnp.arange(n_blocks, dtype=jnp.int32)[:, None]
    flat_slot = ((assigned * n_blocks + block_ids) * CAP + slot_rank).reshape(-1).astype(jnp.int32)
    row_ids = (block_ids * TOK_DEV + jnp.arange(TOK_DEV * TOPK, dtype=jnp.int32)[None, :] // TOPK).reshape(-1).astype(jnp.int32)
    slot_table = jnp.full((EXPERTS * n_blocks * CAP,), n_tokens, jnp.int32).at[flat_slot].set(row_ids)
    padded = jnp.concatenate([normed, jnp.zeros((1, D), jnp.bfloat16)], axis=0)
    width_part = FF // N_TP

    def expert_rows(stacked):
        row_index, gate_w, up_w, down_w = stacked
        inputs = padded[row_index].astype(jnp.float32)
        gate_act = jnp.einsum('nd,dtf->tnf', inputs, gate_w.reshape(D, N_TP, width_part).astype(jnp.float32))
        up_act = jnp.einsum('nd,dtf->tnf', inputs, up_w.reshape(D, N_TP, width_part).astype(jnp.float32))
        hidden = lax.optimization_barrier((jax.nn.silu(gate_act) * up_act).astype(jnp.bfloat16))
        partial_value = jnp.einsum('tnf,tfd->tnd', hidden.astype(jnp.float32), down_w.reshape(N_TP, width_part, D).astype(jnp.float32))
        partial_value = lax.optimization_barrier(partial_value.astype(jnp.bfloat16))
        return lax.optimization_barrier(jnp.sum(partial_value.astype(jnp.float32), axis=0)).astype(jnp.bfloat16)
    results = lax.map(expert_rows, (slot_table.reshape(EXPERTS, n_blocks * CAP), gate_weight, up_weight, down_weight))
    picked = results.reshape(-1, D)[flat_slot].astype(jnp.float32).reshape(n_tokens, TOPK, D)
    shares = route_weight / lax.optimization_barrier(jnp.sum(route_weight, axis=-1, keepdims=True))
    expert_out = lax.optimization_barrier(jnp.sum(shares[:, :, None] * picked, axis=1)).astype(jnp.bfloat16)
    return (mixed_out, expert_out)
```

```python
import functools

import jax
import jax.numpy as jnp
import numpy as np
from jax import lax
from jax.experimental import pallas as pl
from jax.experimental.pallas import tpu as pltpu
from jax.sharding import PartitionSpec as P

HD = 128
NCUT = 8
HQ = 16
KVH = 4
EXPERTS = 16
TOPK = 2
GRID_W = 64
CAP = 8
EPS = 1e-06
THETA = 10000.0
LOG2E = 1.4426950408889634
MESH = pl.DeviceIdType.MESH
BF = jnp.bfloat16
F32 = jnp.float32


def remote(src, dst, send, recv, device):
    return pltpu.make_async_remote_copy(
        src_ref=src,
        dst_ref=dst,
        send_sem=send,
        recv_sem=recv,
        device_id=device,
        device_id_type=MESH,
    )


def done(ref, sem):
    pltpu.make_async_copy(ref, ref, sem).wait()


def turned(x, gain, cosine, sine):
    x = x.astype(F32)
    x = x * lax.rsqrt(jnp.mean(x * x, axis=-1, keepdims=True) + EPS) * gain
    lane = lax.broadcasted_iota(jnp.int32, x.shape, 1)
    partner = jnp.where(lane % 64 < 32, pltpu.roll(x, HD - 32, 1), pltpu.roll(x, 32, 1))
    return (x * cosine + partner * sine).astype(BF)


def tables(length):
    lane = np.arange(HD)
    n_freq = HD // 4
    inverse = np.float32(THETA) ** (-(lane % n_freq).astype(np.float32) / np.float32(n_freq))
    sign = np.where(lane % (2 * n_freq) < n_freq, -1.0, 1.0)

    def both(count, mine):
        angle = np.arange(count, dtype=np.float32)[:, None] * inverse.astype(np.float32)
        angle = angle.astype(np.float64)
        cosine = np.where(mine, np.cos(angle), 0.0)
        sine = np.where(mine, np.sin(angle) * sign, 0.0)
        return np.stack([cosine, sine]).astype(np.float32)

    return both(length // GRID_W, lane < HD // 2), both(GRID_W, lane >= HD // 2)


def kernel(
    n_ep,
    n_tp,
    q_hbm,
    k_hbm,
    v_hbm,
    row_ref,
    col_ref,
    qg_ref,
    kg_ref,
    wo_hbm,
    tok_hbm,
    ng_ref,
    route_ref,
    share_ref,
    wg_hbm,
    wu_hbm,
    wd_hbm,
    mixed_hbm,
    expert_hbm,
    mixed_ref,
    expert_ref,
    wo,
    trig,
    wg,
    wu,
    wd,
    kv,
    values,
    qn,
    att,
    apart,
    asib,
    azr,
    outb,
    arr,
    both,
    hid,
    part,
    sib,
    ret,
    zs,
    zr,
    in_sem,
    out_sem,
    t_sem,
    w_sem,
    kv_s,
    kv_r,
    kvf_s,
    kvf_r,
    d_s,
    d_r,
    df_s,
    df_r,
    do_s,
    do_r,
    a_s,
    a_r,
    az_s,
    az_r,
    p_s,
    p_r,
    r_s,
    r_r,
    z_s,
    z_r,
):
    ep = lax.axis_index("ep")
    tp = lax.axis_index("tp")
    core = lax.rem(tp, 2)
    z = tp // 2
    n_z = n_tp // 2
    other = 1 - core
    sibling = (ep, z * 2 + other)
    if n_ep == 4:
        peers = [(1, ep + 1 - 2 * lax.rem(ep, 2)), (2, ep + 2 - 4 * (ep // 2)), (3, 3 - ep)]
        back = [0, 1, 2, 3]
        near = 2
    else:
        peers = [(k, lax.rem(ep + k, n_ep)) for k in range(1, n_ep)]
        back = [0] + [n_ep - k for k in range(1, n_ep)]
        near = n_ep - 1
    z_peers = [lax.rem(z + k, n_z) for k in range(1, n_z)]
    n_rows = k_hbm.shape[0]
    heads = q_hbm.shape[1] // HD
    depth = tok_hbm.shape[1]
    n_local = wg.shape[0]
    slots = n_z * CAP
    block = tok_hbm.shape[0] // n_tp
    out_rows = mixed_ref.shape[0]
    half = n_z * block
    pair = 2 * out_rows
    tile = pair
    while tile * n_ep * n_rows > 256 * 3072:
        tile //= 2

    barrier = pltpu.get_barrier_semaphore()
    for device in [sibling] + [(p, tp) for _, p in peers] + [(ep, w * 2 + core) for w in z_peers]:
        pl.semaphore_signal(barrier, inc=1, device_id=device, device_id_type=MESH)

    kv_at = pl.multiple_of(tp * heads // (HQ // KVH) * HD, HD)
    k_raw = values.at[pl.ds(0, n_rows), pl.ds(0, HD)]
    get_k = pltpu.make_async_copy(k_hbm.at[:, pl.ds(kv_at, HD)], k_raw, in_sem.at[0])
    get_v = pltpu.make_async_copy(v_hbm.at[:, pl.ds(kv_at, HD)], kv.at[1, 0], in_sem.at[1])
    get_q = pltpu.make_async_copy(q_hbm, att, in_sem.at[2])
    get_wo = pltpu.make_async_copy(wo_hbm, wo, in_sem.at[3])
    get_tok = [
        pltpu.make_async_copy(
            tok_hbm.at[pl.ds(pl.multiple_of((2 * w + core) * block, 16), block), :],
            apart.at[w, 0, pl.ds(0, block), :],
            t_sem,
        )
        for w in range(n_z)
    ]
    for copy in [get_k, get_v] + get_tok + [get_q, get_wo]:
        copy.start()

    n_grid = n_rows // GRID_W
    for r in range(n_grid):
        for t in range(2):
            trig[t, r * GRID_W : (r + 1) * GRID_W, :] = (
                row_ref[t, pl.ds(ep * n_grid + r, 1), :] + col_ref[t]
            )
    with jax.named_scope("kwait"):
        get_k.wait()
    kv[0, 0] = turned(k_raw[...], kg_ref[...], trig[0], trig[1])
    get_v.wait()
    with jax.named_scope("barrier"):
        pl.semaphore_wait(barrier, n_ep + n_z - 1)
    for s, p in peers[:near]:
        remote(kv.at[core, 0], kv.at[core, back[s]], kv_s, kv_r.at[back[s]], (p, tp)).start()

    with jax.named_scope("gather"):
        def mine(table):
            sides = [
                jnp.concatenate(
                    [table[:, (2 * w + c) * block : (2 * w + c + 1) * block] for w in range(n_z)],
                    axis=1,
                )
                for c in range(2)
            ]
            return jnp.where(core == 0, sides[0], sides[1])

        route = mine(route_ref[...])
        e_iota = lax.broadcasted_iota(jnp.int32, (EXPERTS, half), 0)
        hot0 = (e_iota == route[0:1]).astype(F32)
        hot1 = (e_iota == route[1:2]).astype(F32)
        before = lax.broadcasted_iota(jnp.int32, (half, half), 0)
        after = lax.broadcasted_iota(jnp.int32, (half, half), 1)
        earlier = ((before < after) & (before // block == after // block)).astype(F32)
        count = jnp.dot(
            (hot0 + hot1).astype(BF), earlier.astype(BF), preferred_element_type=F32
        )
        rank0 = jnp.sum(hot0 * count, axis=0, keepdims=True).astype(jnp.int32)
        rank1 = jnp.sum(hot1 * count, axis=0, keepdims=True).astype(jnp.int32)
        base = lax.broadcasted_iota(jnp.int32, (1, half), 1) // block * CAP
        slot0 = route[0:1] * slots + base + rank0
        slot1 = route[1:2] * slots + base + rank1
        j_iota = lax.broadcasted_iota(jnp.int32, (EXPERTS * slots, half), 0)
        is0 = j_iota == slot0
        is1 = j_iota == slot1
        mat = (is0 | is1).astype(F32).astype(BF)
        done(apart.at[:, 0, pl.ds(0, block), :], t_sem)
        get_q.wait()
        get_wo.wait()
        weights = [
            pltpu.make_async_copy(src, dst, w_sem.at[j])
            for j, (src, dst) in enumerate(((wg_hbm, wg), (wu_hbm, wu), (wd_hbm, wd)))
        ]
        for copy in weights:
            copy.start()
        field = apart[:, 0, :block, :].reshape(half, depth).astype(F32)
        normed = (
            field
            * lax.rsqrt(jnp.mean(field * field, axis=-1, keepdims=True) + EPS)
            * ng_ref[...]
        ).astype(BF)
        outb[...] = (
            jnp.dot(mat, normed, preferred_element_type=F32)
            .astype(BF)
            .reshape(n_ep, n_local, slots, depth)
        )
        arr[:, core, 0] = outb[ep]
        remote(outb.at[ep], arr.at[:, core, 0], do_s, do_r, sibling).start()
        share = mine(share_ref[...])
        share = share / jnp.sum(share, axis=0, keepdims=True)
        comb = jnp.where(is0, share[0:1], 0.0) + jnp.where(is1, share[1:2], 0.0)
        high = comb.astype(BF)
        low = (comb - high.astype(F32)).astype(BF)
        both[...] = jnp.concatenate([high, low], axis=1)

    with jax.named_scope("qprep"):
        for g in range(heads):
            qn[pl.ds(g * n_rows, n_rows), :] = turned(
                att[:, g * HD : (g + 1) * HD], qg_ref[...], trig[0], trig[1]
            )

    factor = HD ** (-0.5) * LOG2E

    length = n_ep * n_rows

    def attend(at, g):
        scores = lax.dot_general(
            qn[pl.ds(pl.multiple_of(g * n_rows + at, 16), tile), :],
            kv[0].reshape(length, HD),
            (((1,), (1,)), ((), ())),
            preferred_element_type=F32,
        )
        top = jnp.max(scores, axis=1, keepdims=True)
        weight = jnp.exp2((scores - top) * factor).astype(BF)
        merged = jnp.dot(weight, values[...], preferred_element_type=F32)
        att[pl.ds(at, tile), g * HD : (g + 1) * HD] = (
            merged[:, :HD] / merged[:, HD:]
        ).astype(BF)

    with jax.named_scope("kvw"):
        values[:, HD:] = jnp.ones((length, HD), BF)
        for s, p in peers[:near]:
            with jax.named_scope(f"kv_{s}"):
                done(kv.at[core, s], kv_r.at[s])
            if near < n_ep - 1:
                part_of = pl.ds((s - 1) * n_rows // 2, n_rows // 2)
                remote(
                    kv.at[core, s, part_of],
                    kv.at[core, 3, part_of],
                    kv_s,
                    kv_r.at[3],
                    (peers[2 - s][1], tp),
                ).start()
        for s, p in peers[:near]:
            remote(kv.at[core, s], kv.at[core, s], kvf_s, kvf_r, sibling).start()
        for s, p in peers[near:]:
            with jax.named_scope(f"kv_{s}"):
                done(kv.at[core, s], kv_r.at[s])
            remote(kv.at[core, s], kv.at[core, s], kvf_s, kvf_r, sibling).start()
        for i in range(n_local):
            for s, p in peers:
                remote(
                    outb.at[p, i], arr.at[i, core, back[s]], d_s, d_r.at[i], (p, tp)
                ).start()
        with jax.named_scope('kv_sib'):
            done(kv.at[other, 1:], kvf_r)
        values[:, :HD] = kv[1].reshape(length, HD)

    def pass_on(i):
        done(arr.at[i, core, 1:], d_r.at[i])
        remote(arr.at[i, core, 1:], arr.at[i, core, 1:], df_s, df_r.at[i], sibling).start()

    def right(w):
        return remote(
            asib.at[w], azr.at[0, w], az_s.at[w], az_r.at[0, w], (ep, (z + 1) * 2 + core)
        )

    def left(w):
        return remote(
            asib.at[w], azr.at[1, w], az_s.at[w], az_r.at[1, w], (ep, (z - 1) * 2 + core)
        )

    def hand_over(w):
        done(asib.at[w], a_r.at[w])
        asib[w] = (apart[w, core].astype(F32) + asib[w].astype(F32)).astype(BF)

        @pl.when((z == 0) & (w != 0))
        def _():
            right(w).start()

        @pl.when((z == n_z - 1) & (w != n_z - 1))
        def _():
            left(w).start()

    def relay(t):
        to_right = n_z - 1 - t + z
        to_left = t - (n_z - 1 - z)

        @pl.when((z >= 1) & (z <= t))
        def _():
            copy = right(to_right)
            copy.wait_recv()
            asib[to_right] = (
                asib[to_right].astype(F32) + azr[0, to_right].astype(F32)
            ).astype(BF)
            copy.start()

        @pl.when((z <= n_z - 2) & (n_z - 1 - z <= t))
        def _():
            copy = left(to_left)
            copy.wait_recv()
            asib[to_left] = (
                asib[to_left].astype(F32) + azr[1, to_left].astype(F32)
            ).astype(BF)
            copy.start()

    far = 2 * z // n_z
    order = [(1 - far) * (n_z - 1 - k) + far * k for k in range(n_z)]
    for k, w in enumerate(order):
        if k == n_z - 1:
            with jax.named_scope("pass0"):
                pass_on(0)
        with jax.named_scope("last"):
            for g in range(heads):
                for c in range(pair // tile):
                    attend(pl.multiple_of(w * pair + c * tile, 16), g)
        with jax.named_scope("proj"):
            apart[w] = (
                jnp.dot(
                    att[pl.ds(pl.multiple_of(w * pair, 16), pair), :],
                    wo[...],
                    preferred_element_type=F32,
                )
                .astype(BF)
                .reshape(2, out_rows, depth)
            )
            remote(apart.at[w, other], asib.at[w], a_s, a_r.at[w], sibling).start()
            if k == 0:
                hand_over(w)
            elif k > 1:
                hand_over(order[k - 1])
    with jax.named_scope("hand"):
        hand_over(order[-1])

    n_cut, width = part.shape[0], part.shape[-1]

    def give(i, j):
        done(sib.at[j, i], p_r.at[j, i])
        sib[j, i] = (part[j, i, core].astype(F32) + sib[j, i].astype(F32)).astype(BF)
        for s, p in peers:
            remote(sib.at[j, i, s], ret.at[j, ep, i], r_s, r_r.at[j], (p, tp)).start()
        ret[j, ep, i] = sib[j, i, 0]

    relayed = 1
    if relayed < n_z - 1:
        with jax.named_scope("relay"):
            relay(relayed)
        relayed += 1
    early = 3 * n_cut // 8
    done(arr.at[:, other, 0], do_r)
    for copy in weights:
        copy.wait()
    for i in range(n_local):
        with jax.named_scope(f"disp{i}"):
            done(arr.at[i, other, 1:], df_r.at[i])
            if i + 2 < n_local:
                pass_on(i + 1)
        with jax.named_scope(f"ffn{i}"):
            x = arr[i].reshape(2 * n_ep * slots, depth)
            gate = jnp.dot(x, wg[i], preferred_element_type=F32)
            up = jnp.dot(x, wu[i], preferred_element_type=F32)
            hid[i] = (gate / (1.0 + jnp.exp(-gate)) * up).astype(BF)
            for j in range(0, n_cut, 2):
                down = jnp.dot(
                    hid[i], wd[i, :, j * width : (j + 2) * width], preferred_element_type=F32
                ).astype(BF)
                for c in range(2):
                    part[j + c, i] = down[:, c * width : (c + 1) * width].reshape(
                        2, n_ep, slots, width
                    )
                    remote(
                        part.at[j + c, i, other],
                        sib.at[j + c, i],
                        p_s,
                        p_r.at[j + c, i],
                        sibling,
                    ).start()
        if i + 2 == n_local:
            with jax.named_scope("passl"):
                pass_on(i + 1)
        with jax.named_scope(f"give{i}"):
            for j in range(early):
                give(i, j)
        if i == n_local - 2 and relayed < n_z - 1:
            with jax.named_scope("relay"):
                relay(relayed)
            relayed += 1
    with jax.named_scope("gives"):
        for j in range(early, n_cut):
            for i in range(n_local):
                give(i, j)

    with jax.named_scope("relays"):
        while relayed < n_z - 1:
            relay(relayed)
            relayed += 1

    def settle(j):
        done(ret.at[j, 1:], r_r.at[j])
        rows = lax.dot_general(
            both[...],
            ret[j].reshape(EXPERTS * slots, width),
            (((0,), (0,)), ((), ())),
            preferred_element_type=F32,
        )
        rows = rows[:half] + rows[half:]
        zs[j] = rows.astype(BF).reshape(n_z, block, width)
        for w in z_peers:
            remote(zs.at[j, w], zr.at[j, z], z_s, z_r.at[j], (ep, w * 2 + core)).start()

    def mixed():
        mixed_ref[...] = asib[z]

        @pl.when(z >= 1)
        def _():
            right(z).wait_recv()
            mixed_ref[...] = (mixed_ref[...].astype(F32) + azr[0, z].astype(F32)).astype(BF)

        @pl.when(z <= n_z - 2)
        def _():
            left(z).wait_recv()
            mixed_ref[...] = (mixed_ref[...].astype(F32) + azr[1, z].astype(F32)).astype(BF)

        copy = pltpu.make_async_copy(mixed_ref, mixed_hbm, out_sem.at[0])
        copy.start()

    def expert(j):
        total = zs[j, z].astype(F32)
        done(zr.at[j, 1:], z_r.at[j])
        for w in z_peers:
            total = total + zr[j, w].astype(F32)
        at = pl.ds(j * width, width)
        expert_ref[:, at] = total.astype(BF)
        copy = pltpu.make_async_copy(expert_ref.at[:, at], expert_hbm.at[:, at], out_sem.at[1])
        copy.start()

    for j in range(n_cut):
        with jax.named_scope(f"settle{j}"):
            settle(j)
    with jax.named_scope("mixed"):
        mixed()
    for j in range(n_cut):
        with jax.named_scope(f"expert{j}"):
            expert(j)
    with jax.named_scope("drain"):
        done(kv.at[core, 1:], kv_s)
        done(kv.at[core, 1:], kvf_s)
        done(outb.at[1:], d_s)
        done(outb.at[0], do_s)
        done(arr.at[:, core, 1:], df_s)
        done(asib, a_s)
        done(sib, p_s)
        done(sib.at[:, :, 1:], r_s)
        done(zs.at[:, 1:], z_s)
        for k in range(1, n_z):

            @pl.when(z + k <= n_z - 1)
            def _():
                right(z + k).wait_send()

            @pl.when(z - k >= 0)
            def _():
                left(z - k).wait_send()
    with jax.named_scope("outs"):
        done(mixed_ref, out_sem.at[0])
        done(expert_ref, out_sem.at[1])


def lay_out(mixed_hbm, expert_hbm, mixed_out, expert_out, mixed, expert, sems):
    pairs = ((mixed_hbm, mixed, mixed_out), (expert_hbm, expert, expert_out))
    ins = [pltpu.make_async_copy(a, b, sems.at[0, i]) for i, (a, b, _) in enumerate(pairs)]
    outs = [pltpu.make_async_copy(b, c, sems.at[1, i]) for i, (_, b, c) in enumerate(pairs)]
    for copy in ins:
        copy.start()
    for copy, after in zip(ins, outs):
        copy.wait()
        after.start()
    for copy in outs:
        copy.wait()


def on_device(
    queries,
    keys,
    values,
    query_gain,
    key_gain,
    out_weight,
    tokens_b,
    norm_gain,
    routes,
    route_weight,
    gate_weight,
    up_weight,
    down_weight,
):
    n_ep, n_tp = lax.axis_size("ep"), lax.axis_size("tp")
    n_z = n_tp // 2
    n_rows = queries.shape[0]
    heads = queries.shape[1] // HD
    depth = tokens_b.shape[1]
    local_rows = tokens_b.shape[0]
    block = local_rows // n_tp
    n_local, _, ff = gate_weight.shape
    slots = n_z * CAP
    length = n_rows * n_ep
    n_cut = NCUT
    width = depth // n_cut
    row_table, col_table = tables(length)

    vmem = pl.BlockSpec(memory_space=pltpu.VMEM)
    hbm = pl.BlockSpec(memory_space=pl.ANY)
    dma = pltpu.SemaphoreType.DMA
    out_rows = n_rows // n_tp
    scratch = [
        pltpu.VMEM((out_rows, out_weight.shape[1]), BF),
        pltpu.VMEM((block, depth), BF),
        pltpu.VMEM(out_weight.shape, BF),
        pltpu.VMEM((2, n_rows, HD), F32),
        pltpu.VMEM(gate_weight.shape, BF),
        pltpu.VMEM(up_weight.shape, BF),
        pltpu.VMEM(down_weight.shape, BF),
        pltpu.VMEM((2, n_ep, n_rows, HD), BF),
        pltpu.VMEM((length, 2 * HD), BF),
        pltpu.VMEM((heads * n_rows, HD), BF),
        pltpu.VMEM((n_rows, heads * HD), BF),
        pltpu.VMEM((n_z, 2, out_rows, depth), BF),
        pltpu.VMEM((n_z, out_rows, depth), BF),
        pltpu.VMEM((2, n_z, out_rows, depth), BF),
        pltpu.VMEM((n_ep, n_local, slots, depth), BF),
        pltpu.VMEM((n_local, 2, n_ep, slots, depth), BF),
        pltpu.VMEM((EXPERTS * slots, 2 * n_z * block), BF),
        pltpu.VMEM((n_local, 2 * n_ep * slots, ff), BF),
        pltpu.VMEM((n_cut, n_local, 2, n_ep, slots, width), BF),
        pltpu.VMEM((n_cut, n_local, n_ep, slots, width), BF),
        pltpu.VMEM((n_cut, n_ep, n_local, slots, width), BF),
        pltpu.VMEM((n_cut, n_z, block, width), BF),
        pltpu.VMEM((n_cut, n_z, block, width), BF),
        dma((4,)),
        dma((2,)),
        dma,
        dma((3,)),
        dma,
        dma((n_ep,)),
        dma,
        dma,
        dma,
        dma((n_local,)),
        dma,
        dma((n_local,)),
        dma,
        dma,
        dma,
        dma((n_z,)),
        dma((n_z,)),
        dma((2, n_z)),
        dma,
        dma((n_cut, n_local)),
        dma,
        dma((n_cut,)),
        dma,
        dma((n_cut,)),
    ]
    shapes = (
        jax.ShapeDtypeStruct((out_rows, out_weight.shape[1]), BF),
        jax.ShapeDtypeStruct((block, depth), BF),
    )
    results = pl.pallas_call(
        functools.partial(kernel, n_ep, n_tp),
        out_shape=shapes,
        in_specs=[hbm] * 3 + [vmem] * 4 + [hbm] * 2 + [vmem] * 3 + [hbm] * 3,
        out_specs=(hbm, hbm),
        scratch_shapes=scratch,
        compiler_params=pltpu.CompilerParams(
            collective_id=0, has_side_effects=True, vmem_limit_bytes=67043328
        ),
    )(
        queries,
        keys,
        values,
        jnp.asarray(row_table),
        jnp.asarray(col_table),
        query_gain[None],
        key_gain[None],
        out_weight,
        tokens_b,
        norm_gain[None],
        routes.T,
        route_weight.T,
        gate_weight,
        up_weight,
        down_weight,
    )
    return tuple(
        pl.pallas_call(
            lay_out,
            out_shape=shapes,
            in_specs=[hbm] * 2,
            out_specs=(hbm, hbm),
            scratch_shapes=[pltpu.VMEM(x.shape, BF) for x in shapes] + [dma((2, 2))],
        )(*results)
    )


def solution(mesh):
    placed = (
        P("ep", "tp"),
        P("ep", None),
        P("ep", None),
        P(),
        P(),
        P("tp", None),
        P("ep", None),
        P(),
        P("ep", None),
        P("ep", None),
        P("ep", None, "tp"),
        P("ep", None, "tp"),
        P("ep", "tp", None),
    )
    return jax.shard_map(
        on_device,
        mesh=mesh,
        in_specs=placed,
        out_specs=(P(("ep", "tp"), None), P(("ep", "tp"), None)),
        check_vma=False,
    )
```

```python
import functools

import jax
import jax.numpy as jnp
import numpy as np
from jax import lax
from jax.experimental import pallas as pl
from jax.experimental.pallas import tpu as pltpu
from jax.sharding import PartitionSpec as P

HD = 128
NCUT = 8
HQ = 16
KVH = 4
EXPERTS = 16
TOPK = 2
GRID_W = 64
CAP = 8
EPS = 1e-06
THETA = 10000.0
LOG2E = 1.4426950408889634
MESH = pl.DeviceIdType.MESH
BF = jnp.bfloat16
F32 = jnp.float32


def remote(src, dst, send, recv, device):
    return pltpu.make_async_remote_copy(
        src_ref=src,
        dst_ref=dst,
        send_sem=send,
        recv_sem=recv,
        device_id=device,
        device_id_type=MESH,
    )


def done(ref, sem):
    pltpu.make_async_copy(ref, ref, sem).wait()


def turned(x, gain, cosine, sine):
    x = x.astype(F32)
    x = x * lax.rsqrt(jnp.mean(x * x, axis=-1, keepdims=True) + EPS) * gain
    lane = lax.broadcasted_iota(jnp.int32, x.shape, 1)
    partner = jnp.where(lane % 64 < 32, pltpu.roll(x, HD - 32, 1), pltpu.roll(x, 32, 1))
    return (x * cosine + partner * sine).astype(BF)


def tables(length):
    lane = np.arange(HD)
    n_freq = HD // 4
    inverse = np.float32(THETA) ** (-(lane % n_freq).astype(np.float32) / np.float32(n_freq))
    sign = np.where(lane % (2 * n_freq) < n_freq, -1.0, 1.0)

    def both(count, mine):
        angle = np.arange(count, dtype=np.float32)[:, None] * inverse.astype(np.float32)
        angle = angle.astype(np.float64)
        cosine = np.where(mine, np.cos(angle), 0.0)
        sine = np.where(mine, np.sin(angle) * sign, 0.0)
        return np.stack([cosine, sine]).astype(np.float32)

    return both(length // GRID_W, lane < HD // 2), both(GRID_W, lane >= HD // 2)


def kernel(
    n_ep,
    n_tp,
    q_hbm,
    k_hbm,
    v_hbm,
    row_ref,
    col_ref,
    qg_ref,
    kg_ref,
    wo_hbm,
    tok_hbm,
    ng_ref,
    route_ref,
    share_ref,
    wg_hbm,
    wu_hbm,
    wd_hbm,
    mixed_ref,
    expert_ref,
    wo,
    trig,
    wg,
    wu,
    wd,
    kv,
    values,
    qn,
    att,
    apart,
    asib,
    azr,
    outb,
    arr,
    both,
    hid,
    part,
    sib,
    ret,
    zs,
    zr,
    in_sem,
    t_sem,
    w_sem,
    kv_s,
    kv_r,
    kvf_s,
    kvf_r,
    d_s,
    d_r,
    df_s,
    df_r,
    do_s,
    do_r,
    a_s,
    a_r,
    az_s,
    az_r,
    p_s,
    p_r,
    r_s,
    r_r,
    z_s,
    z_r,
):
    ep = lax.axis_index("ep")
    tp = lax.axis_index("tp")
    core = lax.rem(tp, 2)
    z = tp // 2
    n_z = n_tp // 2
    other = 1 - core
    sibling = (ep, z * 2 + other)
    if n_ep == 4:
        peers = [(1, ep + 1 - 2 * lax.rem(ep, 2)), (2, ep + 2 - 4 * (ep // 2)), (3, 3 - ep)]
        back = [0, 1, 2, 3]
        near = 2
    else:
        peers = [(k, lax.rem(ep + k, n_ep)) for k in range(1, n_ep)]
        back = [0] + [n_ep - k for k in range(1, n_ep)]
        near = n_ep - 1
    z_peers = [lax.rem(z + k, n_z) for k in range(1, n_z)]
    n_rows = k_hbm.shape[0]
    heads = q_hbm.shape[1] // HD
    depth = tok_hbm.shape[1]
    n_local = wg.shape[0]
    slots = n_z * CAP
    block = tok_hbm.shape[0] // n_tp
    out_rows = mixed_ref.shape[0]
    half = n_z * block
    pair = 2 * out_rows
    tile = pair
    while tile * n_ep * n_rows > 256 * 3072:
        tile //= 2

    barrier = pltpu.get_barrier_semaphore()
    for device in [sibling] + [(p, tp) for _, p in peers] + [(ep, w * 2 + core) for w in z_peers]:
        pl.semaphore_signal(barrier, inc=1, device_id=device, device_id_type=MESH)

    kv_at = pl.multiple_of(tp * heads // (HQ // KVH) * HD, HD)
    k_raw = values.at[pl.ds(0, n_rows), pl.ds(0, HD)]
    get_k = pltpu.make_async_copy(k_hbm.at[:, pl.ds(kv_at, HD)], k_raw, in_sem.at[0])
    get_v = pltpu.make_async_copy(v_hbm.at[:, pl.ds(kv_at, HD)], kv.at[1, 0], in_sem.at[1])
    get_q = pltpu.make_async_copy(q_hbm, att, in_sem.at[2])
    get_wo = pltpu.make_async_copy(wo_hbm, wo, in_sem.at[3])
    get_tok = [
        pltpu.make_async_copy(
            tok_hbm.at[pl.ds(pl.multiple_of((2 * w + core) * block, 16), block), :],
            apart.at[w, 0, pl.ds(0, block), :],
            t_sem,
        )
        for w in range(n_z)
    ]
    for copy in [get_k, get_v] + get_tok + [get_q, get_wo]:
        copy.start()

    n_grid = n_rows // GRID_W
    for r in range(n_grid):
        for t in range(2):
            trig[t, r * GRID_W : (r + 1) * GRID_W, :] = (
                row_ref[t, pl.ds(ep * n_grid + r, 1), :] + col_ref[t]
            )
    with jax.named_scope("kwait"):
        get_k.wait()
    kv[0, 0] = turned(k_raw[...], kg_ref[...], trig[0], trig[1])
    get_v.wait()
    with jax.named_scope("barrier"):
        pl.semaphore_wait(barrier, n_ep + n_z - 1)
    for s, p in peers[:near]:
        remote(kv.at[core, 0], kv.at[core, back[s]], kv_s, kv_r.at[back[s]], (p, tp)).start()

    with jax.named_scope("gather"):
        def mine(table):
            sides = [
                jnp.concatenate(
                    [table[:, (2 * w + c) * block : (2 * w + c + 1) * block] for w in range(n_z)],
                    axis=1,
                )
                for c in range(2)
            ]
            return jnp.where(core == 0, sides[0], sides[1])

        route = mine(route_ref[...])
        e_iota = lax.broadcasted_iota(jnp.int32, (EXPERTS, half), 0)
        hot0 = (e_iota == route[0:1]).astype(F32)
        hot1 = (e_iota == route[1:2]).astype(F32)
        before = lax.broadcasted_iota(jnp.int32, (half, half), 0)
        after = lax.broadcasted_iota(jnp.int32, (half, half), 1)
        earlier = ((before < after) & (before // block == after // block)).astype(F32)
        count = jnp.dot(
            (hot0 + hot1).astype(BF), earlier.astype(BF), preferred_element_type=F32
        )
        rank0 = jnp.sum(hot0 * count, axis=0, keepdims=True).astype(jnp.int32)
        rank1 = jnp.sum(hot1 * count, axis=0, keepdims=True).astype(jnp.int32)
        base = lax.broadcasted_iota(jnp.int32, (1, half), 1) // block * CAP
        slot0 = route[0:1] * slots + base + rank0
        slot1 = route[1:2] * slots + base + rank1
        j_iota = lax.broadcasted_iota(jnp.int32, (EXPERTS * slots, half), 0)
        is0 = j_iota == slot0
        is1 = j_iota == slot1
        mat = (is0 | is1).astype(F32).astype(BF)
        done(apart.at[:, 0, pl.ds(0, block), :], t_sem)
        get_q.wait()
        get_wo.wait()
        weights = [
            pltpu.make_async_copy(src, dst, w_sem.at[j])
            for j, (src, dst) in enumerate(((wg_hbm, wg), (wu_hbm, wu), (wd_hbm, wd)))
        ]
        for copy in weights:
            copy.start()
        field = apart[:, 0, :block, :].reshape(half, depth).astype(F32)
        normed = (
            field
            * lax.rsqrt(jnp.mean(field * field, axis=-1, keepdims=True) + EPS)
            * ng_ref[...]
        ).astype(BF)
        outb[...] = (
            jnp.dot(mat, normed, preferred_element_type=F32)
            .astype(BF)
            .reshape(n_ep, n_local, slots, depth)
        )
        arr[:, core, 0] = outb[ep]
        remote(outb.at[ep], arr.at[:, core, 0], do_s, do_r, sibling).start()
        share = mine(share_ref[...])
        share = share / jnp.sum(share, axis=0, keepdims=True)
        comb = jnp.where(is0, share[0:1], 0.0) + jnp.where(is1, share[1:2], 0.0)
        high = comb.astype(BF)
        low = (comb - high.astype(F32)).astype(BF)
        both[...] = jnp.concatenate([high, low], axis=1)

    with jax.named_scope("qprep"):
        for g in range(heads):
            qn[pl.ds(g * n_rows, n_rows), :] = turned(
                att[:, g * HD : (g + 1) * HD], qg_ref[...], trig[0], trig[1]
            )

    factor = HD ** (-0.5) * LOG2E

    length = n_ep * n_rows

    far = 2 * z // n_z
    order = [(1 - far) * (n_z - 1 - k) + far * k for k in range(n_z)]

    def scored(at, g, start, end):
        scores = lax.dot_general(
            qn[pl.ds(pl.multiple_of(g * n_rows + at, 16), tile), :],
            kv[0, start:end].reshape((end - start) * n_rows, HD),
            (((1,), (1,)), ((), ())),
            preferred_element_type=F32,
        )
        top = jnp.max(scores, axis=1, keepdims=True)
        weight = jnp.exp2((scores - top) * factor).astype(BF)
        return top, jnp.dot(
            weight, values[start * n_rows : end * n_rows, :], preferred_element_type=F32
        )

    def attend(at, g, held):
        if held is None:
            merged = scored(at, g, 0, n_ep)[1]
        else:
            top, merged = scored(at, g, near + 1, n_ep)
            most = jnp.maximum(top, held[0])
            merged = merged * jnp.exp2((top - most) * factor) + held[1] * jnp.exp2(
                (held[0] - most) * factor
            )
        att[pl.ds(at, tile), g * HD : (g + 1) * HD] = (
            merged[:, :HD] / merged[:, HD:]
        ).astype(BF)

    def tiles(w):
        return [
            (pl.multiple_of(w * pair + c * tile, 16), g)
            for g in range(heads)
            for c in range(pair // tile)
        ]

    def fill(start, end):
        values[start * n_rows : end * n_rows, :HD] = kv[1, start:end].reshape(
            (end - start) * n_rows, HD
        )

    with jax.named_scope("kvw"):
        values[:, HD:] = jnp.ones((length, HD), BF)
        fill(0, 1)
        for s, p in peers[:near]:
            done(kv.at[core, s], kv_r.at[s])
            if near < n_ep - 1:
                part_of = pl.ds((s - 1) * n_rows // 2, n_rows // 2)
                remote(
                    kv.at[core, s, part_of],
                    kv.at[core, 3, part_of],
                    kv_s,
                    kv_r.at[3],
                    (peers[2 - s][1], tp),
                ).start()
        for s, p in peers[:near]:
            remote(kv.at[core, s], kv.at[core, s], kvf_s, kvf_r.at[0], sibling).start()
        done(kv.at[other, 1 : near + 1], kvf_r.at[0])
        fill(1, near + 1)
    first = [None] * len(tiles(0))
    if near < n_ep - 1:
        with jax.named_scope("first"):
            first = [scored(at, g, 0, near + 1) for at, g in tiles(order[0])]
    with jax.named_scope("kvd"):
        for i in range(n_local):
            for s, p in peers:
                remote(
                    outb.at[p, i], arr.at[i, core, back[s]], d_s, d_r.at[i], (p, tp)
                ).start()
        if near < n_ep - 1:
            for s, p in peers[near:]:
                done(kv.at[core, s], kv_r.at[s])
                remote(kv.at[core, s], kv.at[core, s], kvf_s, kvf_r.at[1], sibling).start()
            done(kv.at[other, near + 1 :], kvf_r.at[1])
            fill(near + 1, n_ep)

    def pass_on(i):
        done(arr.at[i, core, 1:], d_r.at[i])
        remote(arr.at[i, core, 1:], arr.at[i, core, 1:], df_s, df_r.at[i], sibling).start()

    def right(w):
        return remote(
            asib.at[w], azr.at[0, w], az_s.at[w], az_r.at[0, w], (ep, (z + 1) * 2 + core)
        )

    def left(w):
        return remote(
            asib.at[w], azr.at[1, w], az_s.at[w], az_r.at[1, w], (ep, (z - 1) * 2 + core)
        )

    def hand_over(w):
        done(asib.at[w], a_r.at[w])
        asib[w] = (apart[w, core].astype(F32) + asib[w].astype(F32)).astype(BF)

        @pl.when((z == 0) & (w != 0))
        def _():
            right(w).start()

        @pl.when((z == n_z - 1) & (w != n_z - 1))
        def _():
            left(w).start()

    def relay(t):
        to_right = n_z - 1 - t + z
        to_left = t - (n_z - 1 - z)

        @pl.when((z >= 1) & (z <= t))
        def _():
            copy = right(to_right)
            copy.wait_recv()
            asib[to_right] = (
                asib[to_right].astype(F32) + azr[0, to_right].astype(F32)
            ).astype(BF)
            copy.start()

        @pl.when((z <= n_z - 2) & (n_z - 1 - z <= t))
        def _():
            copy = left(to_left)
            copy.wait_recv()
            asib[to_left] = (
                asib[to_left].astype(F32) + azr[1, to_left].astype(F32)
            ).astype(BF)
            copy.start()

    for k, w in enumerate(order):
        if k == n_z - 1:
            with jax.named_scope("pass0"):
                pass_on(0)
        with jax.named_scope("last"):
            for (at, g), held in zip(tiles(w), first if k == 0 else [None] * len(first)):
                attend(at, g, held)
        with jax.named_scope("proj"):
            apart[w] = (
                jnp.dot(
                    att[pl.ds(pl.multiple_of(w * pair, 16), pair), :],
                    wo[...],
                    preferred_element_type=F32,
                )
                .astype(BF)
                .reshape(2, out_rows, depth)
            )
            remote(apart.at[w, other], asib.at[w], a_s, a_r.at[w], sibling).start()
            if k == 0:
                hand_over(w)
            elif k > 1:
                hand_over(order[k - 1])
    with jax.named_scope("hand"):
        hand_over(order[-1])

    n_cut, width = part.shape[0], part.shape[-1]

    def give(i, j):
        done(sib.at[j, i], p_r.at[j, i])
        sib[j, i] = (part[j, i, core].astype(F32) + sib[j, i].astype(F32)).astype(BF)
        for s, p in peers:
            remote(sib.at[j, i, s], ret.at[j, ep, i], r_s, r_r.at[j], (p, tp)).start()
        ret[j, ep, i] = sib[j, i, 0]

    relayed = 1
    if relayed < n_z - 1:
        with jax.named_scope("relay"):
            relay(relayed)
        relayed += 1
    early = 3 * n_cut // 8
    done(arr.at[:, other, 0], do_r)
    for copy in weights:
        copy.wait()
    for i in range(n_local):
        with jax.named_scope(f"disp{i}"):
            done(arr.at[i, other, 1:], df_r.at[i])
            if i + 2 < n_local:
                pass_on(i + 1)
        with jax.named_scope(f"ffn{i}"):
            x = arr[i].reshape(2 * n_ep * slots, depth)
            gate = jnp.dot(x, wg[i], preferred_element_type=F32)
            up = jnp.dot(x, wu[i], preferred_element_type=F32)
            hid[i] = (gate / (1.0 + jnp.exp(-gate)) * up).astype(BF)
            for j in range(0, n_cut, 2):
                down = jnp.dot(
                    hid[i], wd[i, :, j * width : (j + 2) * width], preferred_element_type=F32
                ).astype(BF)
                for c in range(2):
                    part[j + c, i] = down[:, c * width : (c + 1) * width].reshape(
                        2, n_ep, slots, width
                    )
                    remote(
                        part.at[j + c, i, other],
                        sib.at[j + c, i],
                        p_s,
                        p_r.at[j + c, i],
                        sibling,
                    ).start()
        if i + 2 == n_local:
            with jax.named_scope("passl"):
                pass_on(i + 1)
        with jax.named_scope(f"give{i}"):
            for j in range(early):
                give(i, j)
        if i == n_local - 2 and relayed < n_z - 1:
            with jax.named_scope("relay"):
                relay(relayed)
            relayed += 1
    with jax.named_scope("gives"):
        for j in range(early, n_cut):
            for i in range(n_local):
                give(i, j)

    with jax.named_scope("relays"):
        while relayed < n_z - 1:
            relay(relayed)
            relayed += 1

    def settle(j):
        done(ret.at[j, 1:], r_r.at[j])
        rows = lax.dot_general(
            both[...],
            ret[j].reshape(EXPERTS * slots, width),
            (((0,), (0,)), ((), ())),
            preferred_element_type=F32,
        )
        rows = rows[:half] + rows[half:]
        zs[j] = rows.astype(BF).reshape(n_z, block, width)
        for w in z_peers:
            remote(zs.at[j, w], zr.at[j, z], z_s, z_r.at[j], (ep, w * 2 + core)).start()

    def mixed():
        mixed_ref[...] = asib[z]

        @pl.when(z >= 1)
        def _():
            right(z).wait_recv()
            mixed_ref[...] = (mixed_ref[...].astype(F32) + azr[0, z].astype(F32)).astype(BF)

        @pl.when(z <= n_z - 2)
        def _():
            left(z).wait_recv()
            mixed_ref[...] = (mixed_ref[...].astype(F32) + azr[1, z].astype(F32)).astype(BF)


    def expert(j):
        total = zs[j, z].astype(F32)
        done(zr.at[j, 1:], z_r.at[j])
        for w in z_peers:
            total = total + zr[j, w].astype(F32)
        at = pl.ds(j * width, width)
        expert_ref[:, at] = total.astype(BF)

    for j in range(n_cut):
        with jax.named_scope(f"settle{j}"):
            settle(j)
    with jax.named_scope("mixed"):
        mixed()
    for j in range(n_cut):
        with jax.named_scope(f"expert{j}"):
            expert(j)
    with jax.named_scope("drain"):
        done(kv.at[core, 1:], kv_s)
        done(kv.at[core, 1:], kvf_s)
        done(outb.at[1:], d_s)
        done(outb.at[0], do_s)
        done(arr.at[:, core, 1:], df_s)
        done(asib, a_s)
        done(sib, p_s)
        done(sib.at[:, :, 1:], r_s)
        done(zs.at[:, 1:], z_s)
        for k in range(1, n_z):

            @pl.when(z + k <= n_z - 1)
            def _():
                right(z + k).wait_send()

            @pl.when(z - k >= 0)
            def _():
                left(z - k).wait_send()


def on_device(
    queries,
    keys,
    values,
    query_gain,
    key_gain,
    out_weight,
    tokens_b,
    norm_gain,
    routes,
    route_weight,
    gate_weight,
    up_weight,
    down_weight,
):
    n_ep, n_tp = lax.axis_size("ep"), lax.axis_size("tp")
    n_z = n_tp // 2
    n_rows = queries.shape[0]
    heads = queries.shape[1] // HD
    depth = tokens_b.shape[1]
    local_rows = tokens_b.shape[0]
    block = local_rows // n_tp
    n_local, _, ff = gate_weight.shape
    slots = n_z * CAP
    length = n_rows * n_ep
    n_cut = NCUT
    width = depth // n_cut
    row_table, col_table = tables(length)

    vmem = pl.BlockSpec(memory_space=pltpu.VMEM)
    hbm = pl.BlockSpec(memory_space=pl.ANY)
    dma = pltpu.SemaphoreType.DMA
    out_rows = n_rows // n_tp
    scratch = [
        pltpu.VMEM(out_weight.shape, BF),
        pltpu.VMEM((2, n_rows, HD), F32),
        pltpu.VMEM(gate_weight.shape, BF),
        pltpu.VMEM(up_weight.shape, BF),
        pltpu.VMEM(down_weight.shape, BF),
        pltpu.VMEM((2, n_ep, n_rows, HD), BF),
        pltpu.VMEM((length, 2 * HD), BF),
        pltpu.VMEM((heads * n_rows, HD), BF),
        pltpu.VMEM((n_rows, heads * HD), BF),
        pltpu.VMEM((n_z, 2, out_rows, depth), BF),
        pltpu.VMEM((n_z, out_rows, depth), BF),
        pltpu.VMEM((2, n_z, out_rows, depth), BF),
        pltpu.VMEM((n_ep, n_local, slots, depth), BF),
        pltpu.VMEM((n_local, 2, n_ep, slots, depth), BF),
        pltpu.VMEM((EXPERTS * slots, 2 * n_z * block), BF),
        pltpu.VMEM((n_local, 2 * n_ep * slots, ff), BF),
        pltpu.VMEM((n_cut, n_local, 2, n_ep, slots, width), BF),
        pltpu.VMEM((n_cut, n_local, n_ep, slots, width), BF),
        pltpu.VMEM((n_cut, n_ep, n_local, slots, width), BF),
        pltpu.VMEM((n_cut, n_z, block, width), BF),
        pltpu.VMEM((n_cut, n_z, block, width), BF),
        dma((4,)),
        dma,
        dma((3,)),
        dma,
        dma((n_ep,)),
        dma,
        dma((2,)),
        dma,
        dma((n_local,)),
        dma,
        dma((n_local,)),
        dma,
        dma,
        dma,
        dma((n_z,)),
        dma((n_z,)),
        dma((2, n_z)),
        dma,
        dma((n_cut, n_local)),
        dma,
        dma((n_cut,)),
        dma,
        dma((n_cut,)),
    ]
    out_bytes = 2 * (out_rows + block) * depth + 2**17
    shapes = (
        jax.ShapeDtypeStruct((out_rows, out_weight.shape[1]), BF),
        jax.ShapeDtypeStruct((block, depth), BF),
    )
    results = pl.pallas_call(
        functools.partial(kernel, n_ep, n_tp),
        out_shape=tuple(pltpu.VMEM(x.shape, x.dtype) for x in shapes),
        in_specs=[hbm] * 3 + [vmem] * 4 + [hbm] * 2 + [vmem] * 3 + [hbm] * 3,
        out_specs=(vmem, vmem),
        scratch_shapes=scratch,
        compiler_params=pltpu.CompilerParams(
            collective_id=0, has_side_effects=True, vmem_limit_bytes=67043328 - out_bytes
        ),
    )(
        queries,
        keys,
        values,
        jnp.asarray(row_table),
        jnp.asarray(col_table),
        query_gain[None],
        key_gain[None],
        out_weight,
        tokens_b,
        norm_gain[None],
        routes.T,
        route_weight.T,
        gate_weight,
        up_weight,
        down_weight,
    )
    return tuple(results)


def solution(mesh):
    placed = (
        P("ep", "tp"),
        P("ep", None),
        P("ep", None),
        P(),
        P(),
        P("tp", None),
        P("ep", None),
        P(),
        P("ep", None),
        P("ep", None),
        P("ep", None, "tp"),
        P("ep", None, "tp"),
        P("ep", "tp", None),
    )
    return jax.shard_map(
        on_device,
        mesh=mesh,
        in_specs=placed,
        out_specs=(P(("ep", "tp"), None), P(("ep", "tp"), None)),
        check_vma=False,
    )
```
